32 devices in a mesh: ep: 8 (over z, y), tp: 4 (over x, core).
Axes of the slice: x: 2, y: 2, z: 4, core: 2. Of those that a mesh axis runs over, the one named last changes fastest.
Arguments:
- tokens: bfloat16 [4096, 2048], P(('ep', 'tp')), may hold values from -6 to 6
- norm_gain: float32 [2048], replicated, may hold values from 0.1 to 1.9
- w_gate: bfloat16 [32, 2048, 512], P(('ep', 'tp')), may hold values from -0.125 to 0.125
- w_up: bfloat16 [32, 2048, 512], P(('ep', 'tp')), may hold values from -0.125 to 0.125
- w_down: bfloat16 [32, 512, 2048], P(('ep', 'tp')), may hold values from -0.25 to 0.25
- routing: int32 [4096, 2], P(('ep', 'tp')), may hold values from 0 to 31, as said below
- gate_weight: float32 [4096, 2], P(('ep', 'tp')), may hold values from 0.05 to 1
Outputs:
- combined: bfloat16 [4096, 2048], P(('ep', 'tp'))
The draws below stay inside these ranges and needn't reach their ends.
Inputs may be any that keep to these rules, and one draw needn't show every extreme that they name: `routing`: A token's 2 experts are distinct and lie in one group of 4 consecutive experts. Of the 128 tokens of each device exactly 16 choose each group; no expert is named by more than 16 tokens of one device, and in every group one expert is named by exactly 16 tokens of every device.
All inputs are finite; a program needn't handle non-finite values.
Results may differ from the reference program's by a relative error of at most 0.0085.
Values may be sent and summed in bfloat16 or wider, within the bound.
No kernel may reach another device: no remote copies, remote signals or barrier semaphores. Data moves between devices by JAX's collectives and lax.ppermute only.
A program may use at most 64 MiB of HBM per device.

```python
import math
import jax
import jax.numpy as jnp
from jax import lax

D = 2048
FF = 512
GROUP_EXPERTS = 4
TOP = 2
TOK_DEV = 128
EXPERTS = 32
GROUPS = 8
CAP = 16
TOKENS = 4096


def draw_routing(key, part):
    source_count = TOKENS // TOK_DEV
    heavy_key = jax.random.fold_in(key, 11)
    cut_key = jax.random.fold_in(key, 12)
    shuffle_key = jax.random.fold_in(key, 13)
    heavy_member = jax.random.randint(heavy_key, (GROUPS,), 0, GROUP_EXPERTS)
    cut_points = jax.random.randint(cut_key, (source_count, GROUPS, 2), 0, CAP + 1)
    lower = jnp.min(cut_points, axis=-1)
    higher = jnp.max(cut_points, axis=-1)
    rest_loads = jnp.stack([lower, higher - lower, CAP - higher], axis=-1)
    members = jnp.arange(GROUP_EXPERTS, dtype=jnp.int32)
    is_heavy = members[None, :] == heavy_member[:, None]
    rank = jnp.clip(members[None, :] - (members[None, :] > heavy_member[:, None]).astype(jnp.int32), 0, 2)
    rank_full = jnp.broadcast_to(rank[None], (source_count, GROUPS, GROUP_EXPERTS))
    load_table = jnp.where(is_heavy[None], CAP, jnp.take_along_axis(rest_loads, rank_full, axis=2))
    bounds = jnp.cumsum(load_table, axis=-1)
    entries = jnp.arange(2 * CAP, dtype=jnp.int32)
    local_ident = jnp.sum((entries[None, None, :, None] >= bounds[:, :, None, :GROUP_EXPERTS - 1]).astype(jnp.int32), axis=-1)
    group_base = jnp.arange(GROUPS, dtype=jnp.int32) * GROUP_EXPERTS
    pair_table = jnp.stack([local_ident[:, :, :CAP], local_ident[:, :, CAP:]], axis=-1) + group_base[None, :, None, None]
    pair_table = pair_table.reshape(source_count, TOK_DEV, TOP)
    shuffles = jax.vmap(lambda subkey: jax.random.permutation(subkey, TOK_DEV))(jax.random.split(shuffle_key, source_count))
    routing = jnp.take_along_axis(pair_table, shuffles[:, :, None].astype(jnp.int32), axis=1)
    return routing.reshape(TOKENS, TOP).astype(jnp.int32)


def level_of(rng, shape, shards, low, top_value):
    level, own = 1.0, jax.random.fold_in(rng, 6)
    for dim, blocks in shards:
        steps = jnp.exp(jax.random.uniform(jax.random.fold_in(own, dim), (blocks,), jnp.float32, low / len(shards), top_value / len(shards)))
        level = level * jnp.repeat(steps, shape[dim] // blocks).reshape([-1 if axis == dim else 1 for axis in range(len(shape))])
    return level


def gaussian(rng, shape, spread, most, cuts=(), kind=jnp.bfloat16):
    values = spread * jax.random.normal(rng, shape, jnp.float32)
    if cuts:
        values = values * level_of(rng, shape, cuts, -0.22, 0.18)
    return jnp.clip(values, -most, most).astype(kind)


def setup_inputs(seed: int = 0) -> dict:
    key_list = jax.random.split(jax.random.key(seed), 8)
    tokens = gaussian(key_list[0], (TOKENS, D), 1.0, 6.0, ((0, 32),))
    norm_gain = jnp.clip(1.0 + 0.18 * jax.random.normal(key_list[1], (D,), jnp.float32), 0.1, 1.9)
    w_gate = gaussian(key_list[2], (EXPERTS, D, FF), D ** -0.5, 0.125, ((0, 32),))
    w_up = gaussian(key_list[3], (EXPERTS, D, FF), D ** -0.5, 0.125, ((0, 32),))
    w_down = gaussian(key_list[4], (EXPERTS, FF, D), FF ** -0.5, 0.25, ((0, 32),))
    routing = draw_routing(jax.random.fold_in(key_list[7], 71), 0)
    gate_weight = jnp.clip(jnp.exp(math.log(1.0) - 2.9957323 * jax.random.uniform(key_list[6], (TOKENS, TOP), jnp.float32) ** level_of(key_list[6], (TOKENS, TOP), ((0, 32),), -0.2, 0.2)), 0.05, 1.0)
    return {"tokens": tokens, "norm_gain": norm_gain, "w_gate": w_gate, "w_up": w_up, "w_down": w_down, "routing": routing, "gate_weight": gate_weight}


def reference(tokens, norm_gain, w_gate, w_up, w_down, routing, gate_weight):
    source_count = TOKENS // TOK_DEV
    values = tokens.astype(jnp.float32)
    scale = lax.rsqrt(lax.optimization_barrier(jnp.mean(values * values, axis=-1, keepdims=True)) + 1e-06)
    normed = (values * scale * norm_gain.astype(jnp.float32)).astype(jnp.bfloat16)
    assigned = routing.reshape(source_count, TOK_DEV * TOP).astype(jnp.int32)

    def count_slots(block):
        onehot = (block[:, None] == jnp.arange(EXPERTS, dtype=jnp.int32)[None, :]).astype(jnp.int32)
        running = jnp.cumsum(onehot, axis=0)
        return lax.optimization_barrier(jnp.sum(onehot * running, axis=1)) - 1
    slot_index = lax.map(count_slots, assigned)
    source_index = jnp.arange(source_count, dtype=jnp.int32)[:, None]
    position = (assigned * source_count + source_index) * CAP + slot_index
    dump_index = TOKENS * TOP
    slot_owner = jnp.full((EXPERTS * source_count * CAP,), dump_index, jnp.int32)
    slot_owner = slot_owner.at[position.reshape(-1)].set(jnp.arange(TOKENS * TOP, dtype=jnp.int32))
    slot_owner = slot_owner.reshape(EXPERTS, source_count * CAP)
    normed_pad = jnp.concatenate([normed, jnp.zeros((1, D), jnp.bfloat16)], axis=0)

    def one_expert(expert, results):
        owners = lax.dynamic_index_in_dim(slot_owner, expert, 0, keepdims=False)
        slot_rows = normed_pad[owners // TOP]
        gate_part = jnp.dot(slot_rows, lax.dynamic_index_in_dim(w_gate, expert, 0, keepdims=False), preferred_element_type=jnp.float32)
        up_part = jnp.dot(slot_rows, lax.dynamic_index_in_dim(w_up, expert, 0, keepdims=False), preferred_element_type=jnp.float32)
        hidden = (jax.nn.silu(gate_part) * up_part).astype(jnp.bfloat16)
        expert_out = jnp.dot(hidden, lax.dynamic_index_in_dim(w_down, expert, 0, keepdims=False), preferred_element_type=jnp.float32).astype(jnp.bfloat16)
        return results.at[owners].set(expert_out)
    results = lax.fori_loop(0, EXPERTS, one_expert, jnp.zeros((TOKENS * TOP + 1, D), jnp.bfloat16))
    picked = results[:TOKENS * TOP].reshape(TOKENS, TOP, D).astype(jnp.float32)
    return lax.optimization_barrier(jnp.sum(gate_weight.astype(jnp.float32)[:, :, None] * picked, axis=1)).astype(jnp.bfloat16)
```

```python
import functools

import jax
import jax.numpy as jnp
from jax import lax
from jax.experimental import pallas as pl
from jax.experimental.pallas import tpu as pltpu
from jax.sharding import PartitionSpec as P


LANES = 128
PARTS = 3
VMEM = pl.BlockSpec(memory_space=pltpu.VMEM)
SMEM = pl.BlockSpec(memory_space=pltpu.SMEM)


def call(kernel, outs, args, flops, scalars=1):
    moved = sum(a.size * a.dtype.itemsize for a in args)
    moved += sum(o.size * o.dtype.itemsize for o in outs)
    return pl.pallas_call(
        kernel,
        out_shape=outs,
        in_specs=[SMEM] * scalars + [VMEM] * (len(args) - scalars),
        out_specs=[VMEM] * len(outs),
        cost_estimate=pl.CostEstimate(flops=flops, bytes_accessed=moved, transcendentals=0),
    )(*args)


def send_kernel(group_bits, cap, me, tok, gain, route, gates, *outs):
    outs, placed = outs[:-1], outs[-1]
    rows, width = tok.shape
    experts = 1 << group_bits
    picks = route[...]
    group = lax.shift_right_logical(picks[:, :1], group_bits) ^ me[0]
    lane = lax.broadcasted_iota(jnp.int32, (rows, LANES), 1)
    chosen = group == lane
    before = lax.broadcasted_iota(jnp.int32, (rows, rows), 0) > lax.broadcasted_iota(
        jnp.int32, (rows, rows), 1
    )
    counts = jnp.dot(
        before.astype(jnp.float32).astype(jnp.bfloat16),
        chosen.astype(jnp.float32).astype(jnp.bfloat16),
        preferred_element_type=jnp.float32,
    )
    rank = jnp.sum(jnp.where(chosen, counts, 0.0), axis=1, keepdims=True)
    slot = group * cap + rank.astype(jnp.int32)
    place = slot == lax.broadcasted_iota(jnp.int32, (rows, rows), 1)
    place = place.astype(jnp.float32)
    placed[...] = place.astype(jnp.bfloat16)
    take = jnp.transpose(place).astype(jnp.bfloat16)

    values = tok[...].astype(jnp.float32)
    scale = lax.rsqrt(jnp.mean(values * values, axis=-1, keepdims=True) + 1e-06)
    normed = (values * scale * gain[...]).astype(jnp.bfloat16)

    member = lane & (experts - 1)
    local = picks & (experts - 1)
    weight = jnp.zeros((rows, LANES), jnp.float32)
    for k in range(picks.shape[1]):
        weight += jnp.where(local[:, k : k + 1] == member, gates[:, k : k + 1], 0.0)
    part = lax.shift_right_logical(lane, group_bits)
    meta = jnp.zeros((rows, LANES), jnp.float32)
    left = weight
    for k in range(PARTS):
        piece = left.astype(jnp.bfloat16).astype(jnp.float32)
        meta = jnp.where(part == k, piece, meta)
        left = left - piece

    body = jnp.dot(take, normed, preferred_element_type=jnp.float32).astype(jnp.bfloat16)
    tail = jnp.dot(
        take, meta.astype(jnp.bfloat16), preferred_element_type=jnp.float32
    ).astype(jnp.bfloat16)
    for k, out in enumerate(outs):
        out[:, :width] = body[k * cap : (k + 1) * cap]
        out[:, width:] = tail[k * cap : (k + 1) * cap]


def join_kernel(cap, *refs):
    ins, out = refs[:-1], refs[-1]
    for k, ref in enumerate(ins):
        out[k * cap : (k + 1) * cap, :] = ref[...]


def expert_kernel(group_bits, me, kept, crossed, kept_c, crossed_c, gate, up, down, own, other):
    experts = 1 << group_bits
    width = gate.shape[1]
    rows = kept.shape[0]
    lane = lax.broadcasted_iota(jnp.int32, (rows, LANES), 1)
    mine = ((lane & (experts - 1)) == me[0]) & (lane < PARTS * experts)
    for ref, out, at in (
        (kept_c, other, 0),
        (crossed_c, other, rows),
        (kept, own, 0),
        (crossed, own, rows),
    ):
        x = ref[:, :width]
        meta = ref[:, width:].astype(jnp.float32)
        weight = jnp.sum(jnp.where(mine, meta, 0.0), axis=1, keepdims=True)
        a = jnp.dot(x, gate[0], preferred_element_type=jnp.float32)
        b = jnp.dot(x, up[0], preferred_element_type=jnp.float32)
        hidden = (a / (1.0 + jnp.exp(-a)) * b).astype(jnp.bfloat16)
        c = jnp.dot(hidden, down[0], preferred_element_type=jnp.float32)
        c = c.astype(jnp.bfloat16).astype(jnp.float32)
        out[at : at + rows, :] = (c * weight).astype(out.dtype)


def pair_kernel(own, got, kept, crossed):
    rows = kept.shape[0]
    total = own[...].astype(jnp.float32) + got[...].astype(jnp.float32)
    kept[...] = total[:rows].astype(kept.dtype)
    crossed[...] = total[rows:].astype(crossed.dtype)


def split_kernel(cap, kept, got, *outs):
    total = kept[...].astype(jnp.float32) + got[...].astype(jnp.float32)
    for k, out in enumerate(outs):
        out[...] = total[k * cap : (k + 1) * cap].astype(out.dtype)


def back_kernel(cap, placed, *refs):
    ins, out = refs[:-1], refs[-1]
    rows = jnp.concatenate([ref[...] for ref in ins], axis=0)
    out[...] = jnp.dot(placed[...], rows, preferred_element_type=jnp.float32).astype(out.dtype)


def local(tokens, norm_gain, w_gate, w_up, w_down, routing, gate_weight):
    rows, width = tokens.shape
    hidden = w_gate.shape[2]
    groups = lax.axis_size("ep")
    members = lax.axis_size("tp")
    bits = members.bit_length() - 1
    cap = rows // groups
    ep = lax.axis_index("ep").reshape(1)
    tp = lax.axis_index("tp").reshape(1)
    bf16 = jnp.bfloat16

    def over(axis, value, bit, size):
        return lax.ppermute(value, axis, [(i, i ^ bit) for i in range(size)])

    def shape(*dims):
        return jax.ShapeDtypeStruct(dims, bf16)

    *blocks, placed = call(
        functools.partial(send_kernel, bits, cap),
        [shape(cap, width + LANES)] * groups + [shape(rows, rows)],
        [ep, tokens, norm_gain.reshape(1, width), routing, gate_weight],
        2 * rows * rows * width,
    )
    waves = [range(groups // 2, groups), range(groups // 2)]
    final = [None] * groups
    sent = {k: (over("ep", blocks[k], k, groups) if k else blocks[k]) for w in waves for k in w}
    for wave in waves:
        count = len(wave) * cap
        (kept,) = call(
            functools.partial(join_kernel, cap),
            [shape(count, width + LANES)],
            [sent[k] for k in wave],
            0,
            0,
        )
        crossed = over("tp", kept, members // 2, members)
        kept_c = over("tp", kept, 1, members)
        crossed_c = over("tp", crossed, 1, members)
        own, other = call(
            functools.partial(expert_kernel, bits),
            [shape(2 * count, width)] * 2,
            [tp, kept, crossed, kept_c, crossed_c, w_gate, w_up, w_down],
            2 * 4 * count * width * hidden * 3,
        )
        got = over("tp", other, 1, members)
        kept, crossed = call(pair_kernel, [shape(count, width)] * 2, [own, got], count * width, 0)
        got = over("tp", crossed, members // 2, members)
        pieces = call(
            functools.partial(split_kernel, cap),
            [shape(cap, width)] * len(wave),
            [kept, got],
            count * width,
            0,
        )
        for k, piece in zip(wave, pieces):
            final[k] = over("ep", piece, k, groups) if k else piece
    (combined,) = call(
        functools.partial(back_kernel, cap),
        [shape(rows, width)],
        [placed] + final,
        2 * rows * rows * width,
        0,
    )
    return combined


def solution(mesh):
    placed = (
        P(("ep", "tp"), None),
        P(),
        P(("ep", "tp"), None, None),
        P(("ep", "tp"), None, None),
        P(("ep", "tp"), None, None),
        P(("ep", "tp"), None),
        P(("ep", "tp"), None),
    )
    return jax.shard_map(
        local, mesh=mesh, in_specs=placed, out_specs=P(("ep", "tp"), None), check_vma=False
    )
```

```python
import functools

import jax
import jax.numpy as jnp
from jax import lax
from jax.experimental import pallas as pl
from jax.experimental.pallas import tpu as pltpu
from jax.sharding import PartitionSpec as P


LANES = 128
PARTS = 3
VMEM = pl.BlockSpec(memory_space=pltpu.VMEM)
SMEM = pl.BlockSpec(memory_space=pltpu.SMEM)


def WAVES(groups):
    return [range(groups // 2, groups), range(groups // 2)]


def call(kernel, outs, args, flops, scalars=0, room=4):
    moved = sum(a.size * a.dtype.itemsize for a in args)
    moved += sum(o.size * o.dtype.itemsize for o in outs)
    return pl.pallas_call(
        kernel,
        out_shape=outs,
        in_specs=[SMEM] * scalars + [VMEM] * (len(args) - scalars),
        out_specs=[VMEM] * len(outs),
        compiler_params=pltpu.CompilerParams(vmem_limit_bytes=room << 20),
        cost_estimate=pl.CostEstimate(flops=flops, bytes_accessed=moved, transcendentals=0),
    )(*args)


def dot(a, b, sides=(1, 0)):
    return lax.dot_general(
        a, b, (((sides[0],), (sides[1],)), ((), ())), preferred_element_type=jnp.float32
    )


def send_kernel(bits, cap, me, tok, gain, route, gates, *outs):
    outs, placed = outs[:-1], outs[-1]
    rows, width = tok.shape
    experts = 1 << bits
    picks = route[...]
    group = lax.shift_right_logical(picks[:1], bits) ^ me[0]
    down = lax.broadcasted_iota(jnp.int32, (rows, rows), 0)
    across = lax.broadcasted_iota(jnp.int32, (rows, rows), 1)
    chosen = group == down
    counts = dot(
        chosen.astype(jnp.float32).astype(jnp.bfloat16),
        (down < across).astype(jnp.float32).astype(jnp.bfloat16),
    )
    rank = jnp.sum(jnp.where(chosen, counts, 0.0), axis=0, keepdims=True)
    slot = group * cap + rank.astype(jnp.int32)
    take = (slot == down).astype(jnp.float32)
    placed[...] = jnp.transpose(take).astype(jnp.bfloat16)
    take = take.astype(jnp.bfloat16)

    values = tok[...].astype(jnp.float32)
    scale = lax.rsqrt(jnp.mean(values * values, axis=-1, keepdims=True) + 1e-06)
    normed = (values * scale * gain[...]).astype(jnp.bfloat16)

    column = lax.broadcasted_iota(jnp.int32, (LANES, rows), 0)
    member = column & (experts - 1)
    local = picks & (experts - 1)
    left = jnp.zeros((LANES, rows), jnp.float32)
    for k in range(picks.shape[0]):
        left += jnp.where(local[k : k + 1] == member, gates[k : k + 1], 0.0)
    part = lax.shift_right_logical(column, bits)
    meta = jnp.zeros((LANES, rows), jnp.float32)
    for k in range(PARTS):
        piece = left.astype(jnp.bfloat16).astype(jnp.float32)
        meta = jnp.where(part == k, piece, meta)
        left = left - piece

    body = dot(take, normed).astype(jnp.bfloat16)
    tail = dot(take, meta.astype(jnp.bfloat16), (1, 1)).astype(jnp.bfloat16)
    for k, out in enumerate(outs):
        out[:, :width] = body[k * cap : (k + 1) * cap]
        out[:, width:] = tail[k * cap : (k + 1) * cap]


def join_kernel(cap, *refs):
    ins, out = refs[:-1], refs[-1]
    for k, ref in enumerate(ins):
        out[k * cap : (k + 1) * cap, :] = ref[...]


def expert_kernel(bits, me, here, there, gate, up, down, own, other):
    experts = 1 << bits
    width = gate.shape[1]
    rows = here.shape[0]
    x = jnp.concatenate([there[:, :width], here[:, :width]], axis=0)
    meta = jnp.concatenate([there[:, width:], here[:, width:]], axis=0).astype(jnp.float32)
    lane = lax.broadcasted_iota(jnp.int32, meta.shape, 1)
    mine = ((lane & (experts - 1)) == me[0]) & (lane < PARTS * experts)
    weight = jnp.sum(jnp.where(mine, meta, 0.0), axis=1, keepdims=True)
    a = dot(x, gate[0])
    b = dot(x, up[0])
    hidden = (a / (1.0 + jnp.exp(-a)) * b).astype(jnp.bfloat16)
    c = dot(hidden, down[0]).astype(jnp.bfloat16).astype(jnp.float32)
    c = (c * weight).astype(jnp.bfloat16)
    other[...] = c[:rows]
    own[...] = c[rows:]


def pair_kernel(own, got, out):
    out[...] = (own[...].astype(jnp.float32) + got[...].astype(jnp.float32)).astype(out.dtype)


def split_kernel(cap, own, near, far, *outs):
    total = own[...].astype(jnp.float32) + near[...].astype(jnp.float32)
    total += far[...].astype(jnp.float32)
    for k, out in enumerate(outs):
        out[...] = total[k * cap : (k + 1) * cap].astype(out.dtype)


def back_kernel(placed, *refs):
    ins, out = refs[:-1], refs[-1]
    rows = jnp.concatenate([ref[...] for ref in ins], axis=0)
    out[...] = dot(placed[...], rows).astype(out.dtype)


def local(tokens, norm_gain, w_gate, w_up, w_down, routing, gate_weight):
    rows, width = tokens.shape
    hidden = w_gate.shape[2]
    groups = lax.axis_size("ep")
    members = lax.axis_size("tp")
    bits = members.bit_length() - 1
    cap = rows // groups
    ep = lax.axis_index("ep").reshape(1)
    tp = lax.axis_index("tp").reshape(1)
    bf16 = jnp.bfloat16

    def over(axis, value, bit, size):
        return lax.ppermute(value, axis, [(i, i ^ bit) for i in range(size)])

    def shape(*dims):
        return jax.ShapeDtypeStruct(dims, bf16)

    *blocks, placed = call(
        functools.partial(send_kernel, bits, cap),
        [shape(cap, width + LANES)] * groups + [shape(rows, rows)],
        [ep, tokens, norm_gain.reshape(1, width), routing.T, gate_weight.T],
        2 * rows * rows * width,
        1,
        8,
    )

    def expert(here, there):
        count = here.shape[0]
        return call(
            functools.partial(expert_kernel, bits),
            [shape(count, width)] * 2,
            [tp, here, there, w_gate, w_up, w_down],
            2 * 2 * count * width * hidden * 3,
            1,
            20,
        )

    waves = WAVES(groups)
    final = [None] * groups
    sent = {k: (over("ep", blocks[k], k, groups) if k else blocks[k]) for w in waves for k in w}
    for wave in waves:
        count = len(wave) * cap
        (kept,) = call(
            functools.partial(join_kernel, cap),
            [shape(count, width + LANES)],
            [sent[k] for k in wave],
            0,
        )
        crossed = over("tp", kept, members // 2, members)
        kept_c = over("tp", kept, 1, members)
        crossed_c = over("tp", crossed, 1, members)
        own_kept, other = expert(kept, kept_c)
        got_kept = over("tp", other, 1, members)
        own_crossed, other = expert(crossed, crossed_c)
        got_crossed = over("tp", other, 1, members)
        (total,) = call(pair_kernel, [shape(count, width)], [own_crossed, got_crossed], 0)
        far = over("tp", total, members // 2, members)
        pieces = call(
            functools.partial(split_kernel, cap),
            [shape(cap, width)] * len(wave),
            [own_kept, got_kept, far],
            count * width,
        )
        for k, piece in zip(wave, pieces):
            final[k] = over("ep", piece, k, groups) if k else piece
    (combined,) = call(
        back_kernel,
        [shape(rows, width)],
        [placed] + final,
        2 * rows * rows * width,
    )
    return combined


def solution(mesh):
    placed = (
        P(("ep", "tp"), None),
        P(),
        P(("ep", "tp"), None, None),
        P(("ep", "tp"), None, None),
        P(("ep", "tp"), None, None),
        P(("ep", "tp"), None),
        P(("ep", "tp"), None),
    )
    return jax.shard_map(
        local, mesh=mesh, in_specs=placed, out_specs=P(("ep", "tp"), None), check_vma=False
    )
```
